32 devices in a mesh: sp: 4 (over y, x), tp: 8 (over z, core).
Axes of the slice: x: 2, y: 2, z: 4, core: 2. Of those that a mesh axis runs over, the one named last changes fastest.
Arguments:
- layer_input: bfloat16 [2048, 2048], P(('sp', 'tp')), may hold values from -6 to 6
- receptance: bfloat16 [2048, 2048], P('sp', 'tp'), may hold values from -6 to 6
- keys: bfloat16 [2048, 2048], P('sp', 'tp'), may hold values from -6 to 6
- values: bfloat16 [2048, 2048], P('sp', 'tp'), may hold values from -6 to 6
- erase_preact: bfloat16 [2048, 2048], P('sp', 'tp'), may hold values from -12 to 5
- decay_preact: bfloat16 [2048, 2048], P('sp', 'tp'), may hold values from -40 to 3
- decay_spike: float32 [2048, 32], P('sp', 'tp'), may hold values from -2 to 0
- head_norm_gain: bfloat16 [2048], P('tp'), may hold values from 0.099609375 to 1.8984375
- output_weight: bfloat16 [2048, 2048], P('tp'), may hold values from -0.125 to 0.125
- expert_norm_gain: bfloat16 [2048], replicated, may hold values from 0.099609375 to 1.8984375
- routes: int32 [2048, 2], P(('sp', 'tp')), may hold values from 0 to 7, all different within a row; in each aligned block of 64 rows (0 to 63, 64 to 127, ...) at most 24 rows name the same one
- routing_weight: float32 [2048, 2], P(('sp', 'tp')), may hold values from 0.3 to 1.5
- expert_gate_weight: bfloat16 [8, 2048, 4096], P('sp', None, 'tp'), may hold values from -0.125 to 0.125
- expert_up_weight: bfloat16 [8, 2048, 4096], P('sp', None, 'tp'), may hold values from -0.125 to 0.125
- expert_down_weight: bfloat16 [8, 4096, 2048], P('sp', 'tp'), may hold values from -0.09375 to 0.09375
- shared_gate_weight: bfloat16 [2048, 4096], P(None, 'tp'), may hold values from -0.125 to 0.125
- shared_up_weight: bfloat16 [2048, 4096], P(None, 'tp'), may hold values from -0.125 to 0.125
- shared_down_weight: bfloat16 [4096, 2048], P('tp'), may hold values from -0.09375 to 0.09375
Outputs:
- layer_out: bfloat16 [2048, 2048], P(('sp', 'tp'))
The draws below stay inside these ranges and needn't reach their ends.
Inputs may be any that keep to these rules, and one draw needn't show every extreme that they name: `routes`: in each aligned block of 64 rows no expert is named by more than 24 rows.
All inputs are finite; a program needn't handle non-finite values.
Results may differ from the reference program's by a relative error of at most 0.02.
Values may be sent and summed in bfloat16 or wider, within the bound.
No kernel may reach another device: no remote copies, remote signals or barrier semaphores. Data moves between devices by JAX's collectives and lax.ppermute only.
A program may use at most 128 MiB of HBM per device.

```python
import math
import jax
import jax.numpy as jnp
import numpy as np
from jax import lax

D = 2048
HEAD = 64
HEADS = 32
TOK_DEV = 512
TOKENS = 2048
ROWS_DEV = 64
EXPERTS = 8
TOP_K = 2
FFE = 4096
SH = 4096
CAP = 24
N_SP = 4
N_TP = 8


def slow_heads(key):
    slow_count = HEADS // 2
    order = jax.random.permutation(jax.random.fold_in(key, 41), HEADS)
    return order < slow_count


def rough_noise(key, array_shape):
    return 0.8 * jax.random.truncated_normal(key, -3.0, 3.0, array_shape, jnp.float32)


def draw_keys(key, part):
    noise = jax.random.normal(jax.random.fold_in(key, 79), (TOKENS, D), jnp.float32)
    common = jax.random.normal(jax.random.fold_in(key, 73), (1, D), jnp.float32)
    return jnp.clip(common + noise, -6.0, 6.0).astype(jnp.bfloat16)


def draw_decay_preact(key, part):
    slow = slow_heads(key)
    fast_rate = jax.random.uniform(jax.random.fold_in(key, 43), (HEADS,), jnp.float32, 0.01, 0.033)
    head_rate = jnp.where(slow, 0.1 / TOKENS, fast_rate)
    head_base = jnp.repeat(jnp.log(head_rate) + 0.5, HEAD)[None, :]
    stretch = jax.random.uniform(jax.random.fold_in(key, 47), (TOKENS // TOK_DEV, 1), jnp.float32, -0.7, 0.7)
    per_block = jnp.repeat(stretch, TOK_DEV, axis=0)
    noise = rough_noise(jax.random.fold_in(key, 53), (TOKENS, D))
    return (head_base + per_block + noise).astype(jnp.bfloat16)


def draw_erase_preact(key, part):
    slow = slow_heads(key)
    fast_base = jax.random.uniform(jax.random.fold_in(key, 59), (HEADS,), jnp.float32, 2.0, 2.6)
    head_base = jnp.repeat(jnp.where(slow, -7.0, fast_base), HEAD)[None, :]
    noise = rough_noise(jax.random.fold_in(key, 61), (TOKENS, D))
    return jnp.clip(head_base + noise, -12.0, 5.0).astype(jnp.bfloat16)


def draw_decay_spike(key, part):
    where_hit = jax.random.randint(jax.random.fold_in(key, 67), (3,), 0, TOKENS)
    depth = jnp.log(jax.random.uniform(jax.random.fold_in(key, 71), (3, HEADS), jnp.float32, 0.5, 0.8))
    hits = (jnp.arange(TOKENS, dtype=jnp.int32)[:, None] == where_hit[None, :]).astype(jnp.float32)
    return jnp.dot(hits, depth)


def levels(rng, shape, split, low, largest):
    def one(dim, blocks):
        steps = jax.random.uniform(jax.random.fold_in(jax.random.fold_in(rng, 6), dim), (blocks,), jnp.float32, low / len(split), largest / len(split))
        return jnp.repeat(jnp.exp(steps), shape[dim] // blocks).reshape((-1,) + (1,) * (len(shape) - dim - 1))

    factor_of = one(*split[0])
    for cut in split[1:]:
        factor_of = factor_of * one(*cut)
    return factor_of


def routed_block(key, own, number, rows, amount, top, bound, skew):
    sequence = jax.random.permutation(key, amount)
    packed, ordinary = shares(amount, rows * top, bound, skew, True), shares(amount, rows * top, bound, skew, False)
    places = jnp.arange(amount)

    def named(sizes, turn):
        used = int((sizes > 0).sum())
        fixed = max(1, used // 4)
        shifted = fixed + (places - fixed + turn * (used - fixed)) % max(1, amount - fixed)
        return jnp.zeros((amount,), jnp.int32).at[sequence[jnp.where(places < fixed, places, shifted)]].set(jnp.asarray(sizes, jnp.int32))

    sizes = jnp.where(number % 4 == 0, named(packed, number // 4), named(ordinary, number - number // 4 - 1))
    mixed = jax.random.permutation(jax.random.fold_in(own, 3), amount)
    giver, taker = mixed[0:amount // 2 * 2:2], mixed[1:amount // 2 * 2:2]
    margin = jnp.minimum(sizes[giver] - 1, bound - sizes[taker]) // 2
    margin = jnp.where((giver == sequence[0]) | (taker == sequence[0]) | (sizes[taker] == 0), 0, jnp.maximum(margin, 0))
    shifted = jax.random.randint(jax.random.fold_in(own, 4), (amount // 2,), 0, 1 << 20) % (margin + 1)
    sizes = sizes.at[giver].add(-shifted).at[taker].add(shifted)
    members = jnp.searchsorted(jnp.cumsum(sizes), jnp.arange(rows * top), side="right").astype(jnp.int32)
    table = members.reshape(top, rows).T
    table = table[jax.random.permutation(jax.random.fold_in(own, 1), rows)]
    turn = jax.random.randint(jax.random.fold_in(own, 2), (rows, 1), 0, top)
    return jnp.take_along_axis(table, (jnp.arange(top)[None, :] + turn) % top, axis=1)


def shares(number_of, total, bound, skew, full):
    loads = [(1 << 20) // math.isqrt(standing ** skew) + 1 for standing in range(1, number_of + 1)]
    largest = bound if full else min(bound, max(-(-total // number_of), total * loads[0] // sum(loads)))
    least = 1 if total - largest >= number_of - 1 else 0
    given, surplus = [largest] + [least] * (number_of - 1), total - largest - least * (number_of - 1)
    while surplus > 0:
        free = [i for i in range(1, number_of) if given[i] < largest] or [i for i in range(1, number_of) if given[i] < bound]
        pool, remaining = sum([loads[i] for i in free]), surplus
        for i in free:
            extra = min(bound - given[i], max(1, remaining * loads[i] // pool), surplus)
            given[i] = given[i] + extra
            surplus = surplus - extra
    return np.array(given)


def bell_draw(rng, dims, scale, reach, cuts=(), kind=jnp.bfloat16):
    factor_of = levels(rng, dims, cuts, -0.22, 0.18) if cuts else 1.0
    drawn = jax.random.normal(rng, dims, jnp.float32) * scale * factor_of
    return jnp.minimum(jnp.maximum(drawn, -reach), reach).astype(kind)


def setup_inputs(seed: int = 0) -> dict:
    key_list = jax.random.split(jax.random.key(seed), 19)
    layer_input = bell_draw(key_list[0], (TOKENS, D), 1.0, 6.0, ((0, 32),))
    receptance = bell_draw(key_list[1], (TOKENS, D), 1.0, 6.0, ((0, 4), (1, 8)))
    keys = draw_keys(jax.random.fold_in(key_list[18], 71), 0)
    values = bell_draw(key_list[3], (TOKENS, D), 1.0, 6.0, ((0, 4), (1, 8)))
    erase_preact = draw_erase_preact(jax.random.fold_in(key_list[18], 71), 0)
    decay_preact = draw_decay_preact(jax.random.fold_in(key_list[18], 71), 0)
    decay_spike = draw_decay_spike(jax.random.fold_in(key_list[18], 71), 0)
    head_norm_gain = jnp.clip(1.0 + 0.18 * jax.random.normal(key_list[7], (D,), jnp.float32), 0.099609375, 1.8984375).astype(jnp.bfloat16)
    output_weight = bell_draw(key_list[8], (D, D), D ** -0.5, 0.125, ((0, 8),))
    expert_norm_gain = jnp.clip(1.0 + 0.18 * jax.random.normal(key_list[9], (D,), jnp.float32), 0.099609375, 1.8984375).astype(jnp.bfloat16)
    routes_keys = jax.random.split(jax.random.fold_in(key_list[10], 1), TOKENS // ROWS_DEV)
    routes_turns = jax.random.permutation(jax.random.fold_in(key_list[10], 3), TOKENS // ROWS_DEV)
    routes = jax.vmap(lambda own, number: routed_block(jax.random.fold_in(key_list[10], 2), own, number, ROWS_DEV, EXPERTS, TOP_K, CAP, 2))(routes_keys, routes_turns).reshape((TOKENS, TOP_K))
    routing_weight = jnp.clip(0.3 + 1.2 * jax.random.uniform(key_list[11], (TOKENS, TOP_K), jnp.float32) ** levels(key_list[11], (TOKENS, TOP_K), ((0, 32),), -0.2, 0.2), 0.3, 1.5)
    expert_gate_weight = bell_draw(key_list[12], (EXPERTS, D, FFE), D ** -0.5, 0.125, ((0, 4), (2, 8)))
    expert_up_weight = bell_draw(key_list[13], (EXPERTS, D, FFE), D ** -0.5, 0.125, ((0, 4), (2, 8)))
    expert_down_weight = bell_draw(key_list[14], (EXPERTS, FFE, D), FFE ** -0.5, 0.09375, ((0, 4), (1, 8)))
    shared_gate_weight = bell_draw(key_list[15], (D, SH), D ** -0.5, 0.125, ((1, 8),))
    shared_up_weight = bell_draw(key_list[16], (D, SH), D ** -0.5, 0.125, ((1, 8),))
    shared_down_weight = bell_draw(key_list[17], (SH, D), SH ** -0.5, 0.09375, ((0, 8),))
    return dict(layer_input=layer_input, receptance=receptance, keys=keys, values=values, erase_preact=erase_preact, decay_preact=decay_preact, decay_spike=decay_spike, head_norm_gain=head_norm_gain, output_weight=output_weight, expert_norm_gain=expert_norm_gain, routes=routes, routing_weight=routing_weight, expert_gate_weight=expert_gate_weight, expert_up_weight=expert_up_weight, expert_down_weight=expert_down_weight, shared_gate_weight=shared_gate_weight, shared_up_weight=shared_up_weight, shared_down_weight=shared_down_weight)


highest = lax.Precision.HIGHEST
GN_EPS = 0.00064
RMS_EPS = 1e-06

def each_head(array):
    return array.astype(jnp.float32).reshape(array.shape[0], HEADS, HEAD)

def recurrence(decay_factor, unit_keys, beta, key_rows, value_rows, read_rows):

    def advance(state_now, inputs):
        decay_t, unit_t, beta_t, key_t, value_t, read_t = inputs
        removed = jnp.einsum('hij,hj->hi', state_now, unit_t, precision=highest)
        state_now = state_now * decay_t[:, None, :] - removed[:, :, None] * beta_t[:, None, :] + value_t[:, :, None] * key_t[:, None, :]
        return (state_now, jnp.einsum('hij,hj->hi', state_now, read_t, precision=highest))
    start_state = jnp.zeros((HEADS, HEAD, HEAD), jnp.float32)
    _, outputs = lax.scan(advance, start_state, (decay_factor, unit_keys, beta, key_rows, value_rows, read_rows))
    return outputs

def grouped_down(hidden, down, groups):
    group_cols = hidden.shape[1] // groups

    def add_group(running, group_idx):
        first_col = (group_idx * group_cols).astype(jnp.int32)
        hidden_part = lax.dynamic_slice_in_dim(hidden, first_col, group_cols, 1)
        down_part = lax.dynamic_slice_in_dim(down, first_col, group_cols, 0)
        partial_value = jnp.dot(hidden_part, down_part, preferred_element_type=jnp.float32).astype(jnp.bfloat16)
        partial_value = lax.optimization_barrier(partial_value)
        return (running + partial_value.astype(jnp.float32), None)
    running, _ = lax.scan(add_group, jnp.zeros((hidden.shape[0], down.shape[1]), jnp.float32), jnp.arange(groups, dtype=jnp.int32))
    return running

def reference(layer_input, receptance, keys, values, erase_preact, decay_preact, decay_spike, head_norm_gain, output_weight, expert_norm_gain, routes, routing_weight, expert_gate_weight, expert_up_weight, expert_down_weight, shared_gate_weight, shared_up_weight, shared_down_weight):
    key_rows = each_head(keys)
    unit_keys = key_rows * lax.rsqrt(lax.optimization_barrier(jnp.sum(key_rows * key_rows, axis=-1, keepdims=True)) + 1e-06)
    beta = unit_keys * jax.nn.sigmoid(each_head(erase_preact))
    decay_factor = jnp.exp(-jnp.exp(-jax.nn.softplus(-each_head(decay_preact)) - 0.5) + decay_spike.astype(jnp.float32)[:, :, None])
    value_rows = each_head(values)
    read_rows = each_head(receptance)
    forward = recurrence(decay_factor, unit_keys, beta, key_rows, value_rows, read_rows)
    flipped = [array[::-1] for array in (decay_factor, unit_keys, beta, key_rows, value_rows, read_rows)]
    backward = recurrence(*flipped)[::-1]
    mix = forward + backward
    center = lax.optimization_barrier(jnp.mean(mix, axis=-1, keepdims=True))
    spread = lax.optimization_barrier(jnp.mean(jnp.square(mix - center), axis=-1, keepdims=True))
    mixed = ((mix - center) * lax.rsqrt(spread + GN_EPS)).reshape(TOKENS, D) * head_norm_gain.astype(jnp.float32)
    mixed = mixed.astype(jnp.bfloat16)
    residual = layer_input.astype(jnp.float32) + jnp.dot(mixed, output_weight, preferred_element_type=jnp.float32)
    normed = residual * lax.rsqrt(lax.optimization_barrier(jnp.mean(residual * residual, axis=-1, keepdims=True)) + RMS_EPS)
    normed = (normed * expert_norm_gain.astype(jnp.float32)).astype(jnp.bfloat16)
    shared_hidden = (jax.nn.silu(jnp.dot(normed, shared_gate_weight, preferred_element_type=jnp.float32)) * jnp.dot(normed, shared_up_weight, preferred_element_type=jnp.float32)).astype(jnp.bfloat16)
    shared = grouped_down(shared_hidden, shared_down_weight, N_TP)
    entries = routes.reshape(-1).astype(jnp.int32)
    entry_weight = routing_weight.reshape(-1).astype(jnp.float32)
    entry_owner = jnp.arange(TOKENS * TOP_K, dtype=jnp.int32) // TOP_K
    most_rows = N_SP * N_TP * CAP

    def one_expert(running, expert):
        chosen = entries == expert
        position = jnp.cumsum(chosen.astype(jnp.int32)) - 1
        target = jnp.where(chosen, position, most_rows).astype(jnp.int32)
        owners = jnp.full((most_rows,), TOKENS, jnp.int32).at[target].set(entry_owner, mode='drop')
        weights = jnp.zeros((most_rows,), jnp.float32).at[target].set(entry_weight, mode='drop')
        picked = jnp.take(normed, jnp.minimum(owners, TOKENS - 1).astype(jnp.int32), axis=0)
        gate_value = jnp.dot(picked, expert_gate_weight[expert], preferred_element_type=jnp.float32)
        up_value = jnp.dot(picked, expert_up_weight[expert], preferred_element_type=jnp.float32)
        hidden = (jax.nn.silu(gate_value) * up_value).astype(jnp.bfloat16)
        routed = grouped_down(hidden, expert_down_weight[expert], N_TP).astype(jnp.bfloat16)
        routed = lax.optimization_barrier(routed)
        running = running.at[owners].add(weights[:, None] * routed.astype(jnp.float32), mode='drop')
        return (running, None)
    routed_sum, _ = lax.scan(one_expert, jnp.zeros((TOKENS, D), jnp.float32), jnp.arange(EXPERTS, dtype=jnp.int32))
    return (residual + shared + routed_sum).astype(jnp.bfloat16)
```

```python
import functools
import jax
import jax.numpy as jnp
from jax import lax
from jax.experimental import pallas as pl
from jax.experimental.pallas import tpu as pltpu
from jax.sharding import PartitionSpec as P

highest = lax.Precision.HIGHEST

GN_EPS = 0.00064
RMS_EPS = 1e-06
LANES = 128
F32, BF16 = jnp.float32, jnp.bfloat16


def split(x):
    high = x.astype(BF16)
    return high, (x - high.astype(F32)).astype(BF16)


def dot(x, y):
    return jnp.dot(x, y, preferred_element_type=F32)


def dot_nt(x, y):
    return lax.dot_general(x, y, (((1,), (1,)), ((), ())), preferred_element_type=F32)


def head_of_lane(shape, head):
    return lax.broadcasted_iota(jnp.int32, shape, len(shape) - 1) // head


def expand(x, head):
    which = head_of_lane(x.shape, head)
    zero = jnp.zeros_like(x)
    return jnp.concatenate([jnp.where(which == h, x, zero) for h in range(x.shape[1] // head)], axis=0)


def wide(y, head):
    high, low = split(y)
    return jnp.concatenate([expand(high, head), expand(low, head)], axis=1)


def tall(x):
    high, low = split(x)
    return jnp.concatenate([high, low], axis=0)


def fold(out, rows, columns=LANES):
    return out[:rows, :columns] + (out[rows:, :columns] + out[:rows, columns:])


def times(x, y, head):
    return fold(dot(tall(x), wide(y, head)), x.shape[0])


def mixer_kernel(head, group, r_ref, k_ref, v_ref, e_ref, d_ref, s_ref,
                 loc_ref, rpf_ref, rpb_ref, maps_ref, ro_ref, pc_ref):
    tokens, width = k_ref.shape
    pairs, span = width // LANES, head
    per = LANES // head
    blocks = tokens // span
    row = lax.broadcasted_iota(jnp.int32, (span, LANES), 0)
    lane = lax.broadcasted_iota(jnp.int32, (span, LANES), 1)
    col = lane % head
    which = lane // head
    eye = (row == col).astype(F32)
    ones_bd = expand(jnp.ones((head, LANES), BF16), head)
    tri_row = lax.broadcasted_iota(jnp.int32, (span, span), 0)
    tri_col = lax.broadcasted_iota(jnp.int32, (span, span), 1)
    tri = (tri_row >= tri_col).astype(BF16)
    tri3 = jnp.concatenate([tri, tri, tri], axis=1)

    def prepare(at, p):
        lanes = slice(p * LANES, (p + 1) * LANES)
        rows = pl.ds(pl.multiple_of(at * span, span), span)
        keys = k_ref[rows, lanes].astype(F32)
        square = keys * keys
        total = dot(tall(square), ones_bd)
        unit = keys * lax.rsqrt(total[:span] + total[span:] + 1e-06)
        beta = unit / (1.0 + jnp.exp(-e_ref[rows, lanes].astype(F32)))
        spike = s_ref[rows, p * per:p * per + 1]
        for h in range(1, per):
            spike = jnp.where(which == h, s_ref[rows, p * per + h:p * per + h + 1], spike)
        log_decay = spike - 0.6065306597126334 / (1.0 + jnp.exp(-d_ref[rows, lanes].astype(F32)))
        high = log_decay.astype(BF16)
        rest = log_decay - high.astype(F32)
        mid = rest.astype(BF16)
        low = (rest - mid.astype(F32)).astype(BF16)
        cum = dot(tri3, jnp.concatenate([high, mid, low], axis=0))
        before = cum - log_decay
        centre, end = cum[span // 2 - 1:span // 2], cum[span - 1:span]
        e1, e0 = jnp.exp(cum - centre), jnp.exp(before - centre)
        i1, i0 = jnp.exp(centre - cum), jnp.exp(centre - before)
        fa, fb, fe = jnp.exp(centre), jnp.exp(end - centre), jnp.exp(end)
        read = r_ref[rows, lanes].astype(F32)
        forward = dict(u=unit * e0, r=read * e1, b=beta * i1, k=keys * i1, start=fa, total=fb)
        backward = dict(u=unit * i1, r=read * i0, b=beta * e0, k=keys * e0, start=fb, total=fa)
        for d, unit_of in ((0, forward), (1, backward)):
            unit_of.update(end=fe, v=v_ref[rows, lanes], at=at, p=p, d=d, lanes=lanes, rows=rows)
        return [forward, backward]

    same = [(row // (8 << i)) == (col // (8 << i)) for i in range(8) if (8 << i) <= span]
    strict = (row > col, row < col)
    incl = (row >= col, row <= col)

    def one_group(i, carry):
        units = []
        for g in range(group):
            for p in range(pairs):
                units += prepare(i * group + g, p)
        for q in units:
            left = tall(jnp.concatenate([q["u"], q["r"], eye * q["total"]], axis=0))
            bh, bl = split(q["b"])
            kh, kl = split(q["k"])
            right = jnp.concatenate([expand(x, head) for x in (bh, bl)], axis=0)
            out = fold(dot_nt(left, right), 3 * span)
            q["ub"] = jnp.where(strict[q["d"]], out[:span], 0.0)
            q["rb"] = jnp.where(incl[q["d"]], out[span:2 * span], 0.0)
            q["be"] = out[2 * span:]
            right = jnp.concatenate([expand(x, head) for x in (kh, kl)], axis=0)
            out = fold(dot_nt(left, right), 3 * span)
            q["uk"] = jnp.where(strict[q["d"]], out[:span], 0.0)
            q["rk"] = jnp.where(incl[q["d"]], out[span:2 * span], 0.0)
            q["ke"] = out[2 * span:]
        for q in units:
            q["D"] = jnp.where(same[0], q["ub"], 0.0)
            q["x"] = eye - q["D"]
        for q in units:
            q["D2"] = times(q["D"], q["D"], head)
        for q in units:
            left = jnp.concatenate([q["x"], q["D2"]], axis=0)
            out = times(left, q["D2"], head)
            q["x"], q["D4"] = q["x"] + out[:span], out[span:]
        for q in units:
            q["x"] = q["x"] + times(q["x"], q["D4"], head)
        for level in range(1, len(same)):
            for q in units:
                off = jnp.where(same[level] & ~same[level - 1], q["ub"], 0.0)
                q["t"] = times(q["x"], off, head)
            for q in units:
                q["x"] = q["x"] - times(q["t"], q["x"], head)
        for q in units:
            left = tall(jnp.concatenate([q["uk"], q["rk"], q["ke"]], axis=0))
            out = dot(left, expand(q["v"], head))
            out = out[:3 * span] + out[3 * span:]
            q["ukv"], q["rkv"], q["kev"] = out[:span], out[span:2 * span], out[2 * span:]
        for q in units:
            left = tall(q["x"])
            q["w"] = fold(dot(left, wide(q["u"] * q["start"], head)), span)
            q["y"] = fold(dot(left, wide(-q["ukv"], head)), span)
        for q in units:
            left = tall(jnp.concatenate([q["rb"], q["be"]], axis=0))
            ow = fold(dot(left, wide(q["w"], head)), 2 * span)
            oy = fold(dot(left, wide(q["y"], head)), 2 * span)
            readout = q["r"] * q["start"] - ow[:span]
            local = oy[:span] + q["rkv"]
            step = eye * q["end"] - ow[span:]
            carried = oy[span:] + q["kev"]
            at = (q["d"] * pairs + q["p"]) * blocks + q["at"]
            ro_ref[at, :span] = step
            ro_ref[at, span:] = readout
            pc_ref[at] = carried
            if q["d"] == 0:
                q_first = local
            else:
                loc_ref[q["rows"], q["lanes"]] = q_first + local
        return carry

    lax.fori_loop(0, blocks // group, one_group, 0)

    start = tuple(
        (jnp.zeros((span, LANES), F32), eye) for _ in range(2 * pairs)
    )

    def advance(i, states):
        after = []
        for c, (state, product) in enumerate(states):
            d, p = c // pairs, c % pairs
            at = i if d == 0 else blocks - 1 - i
            lanes = slice(p * LANES, (p + 1) * LANES)
            rows = pl.ds(pl.multiple_of(at * span, span), span)
            left = tall(ro_ref[c * blocks + at])
            zs = fold(dot(left, wide(state, head)), 2 * span)
            ps = fold(dot(left, wide(product, head)), 2 * span)
            loc_ref[rows, lanes] += zs[span:]
            (rpf_ref, rpb_ref)[d][rows, lanes] = ps[span:]
            after.append((zs[:span] + pc_ref[c * blocks + at], ps[:span]))
        return tuple(after)

    states = lax.fori_loop(0, blocks, advance, start)
    for c, (state, product) in enumerate(states):
        maps_ref[c, 0] = state.astype(BF16)
        maps_ref[c, 1] = product.astype(BF16)


def finish_kernel(head, count, place_ref, maps_ref, loc_ref, rpf_ref, rpb_ref, gain_ref, out_ref):
    tokens, width = loc_ref.shape
    pairs = width // LANES
    place = place_ref[0]
    entries = []
    for c in range(2 * pairs):
        state = jnp.zeros((head, LANES), F32)
        for far in range(count - 1, 0, -1):
            s = far if c < pairs else count - far
            reached = (place >= far) if c < pairs else (place + far < count)
            out = dot(maps_ref[s - 1, c, 1], wide(state, head))
            new = out[:, :LANES] + out[:, LANES:] + maps_ref[s - 1, c, 0].astype(F32)
            state = jnp.where(reached, new, state)
        entries.append(state)
    mean_bd = expand(jnp.full((head, LANES), 1.0 / head, BF16), head)
    for p in range(pairs):
        lanes = slice(p * LANES, (p + 1) * LANES)
        mix = (
            loc_ref[:, lanes]
            + times(rpf_ref[:, lanes], entries[p], head)
            + times(rpb_ref[:, lanes], entries[pairs + p], head)
        )
        total = dot(tall(mix), mean_bd)
        away = mix - (total[:tokens] + total[tokens:])
        total = dot(tall(away * away), mean_bd)
        scaled = away * lax.rsqrt(total[:tokens] + total[tokens:] + GN_EPS)
        out_ref[:, lanes] = (scaled * gain_ref[:, lanes].astype(F32)).astype(BF16)


def vmem_call(kernel, out_shape, scratch=(), scalars=0, flops=0, limit=48 << 20):
    many = isinstance(out_shape, (tuple, list))
    return lambda *args: pl.pallas_call(
        kernel,
        out_shape=out_shape,
        in_specs=[pl.BlockSpec(memory_space=pltpu.SMEM)] * scalars
        + [pl.BlockSpec(memory_space=pltpu.VMEM)] * (len(args) - scalars),
        out_specs=jax.tree.map(lambda _: pl.BlockSpec(memory_space=pltpu.VMEM), out_shape),
        scratch_shapes=list(scratch),
        compiler_params=pltpu.CompilerParams(vmem_limit_bytes=limit),
        cost_estimate=pl.CostEstimate(flops=flops, bytes_accessed=4 << 20, transcendentals=0),
    )(*args)


def mixer(receptance, keys, values, erase_preact, decay_preact, decay_spike, head_norm_gain):
    tokens, width = keys.shape
    head = width // decay_spike.shape[1]
    pairs, blocks = width // LANES, tokens // head
    count, place = lax.axis_size("sp"), lax.axis_index("sp")
    shape = jax.ShapeDtypeStruct((tokens, width), F32)
    group = 2 if blocks % 2 == 0 else 1
    local, read_f, read_b, maps = vmem_call(
        functools.partial(mixer_kernel, head, group),
        (shape, shape, shape, jax.ShapeDtypeStruct((2 * pairs, 2, head, LANES), BF16)),
        [
            pltpu.VMEM((2 * pairs * blocks, 2 * head, LANES), F32),
            pltpu.VMEM((2 * pairs * blocks, head, LANES), F32),
        ],
        flops=20_000_000_000,
    )(receptance, keys, values, erase_preact, decay_preact, decay_spike)
    arrived = [
        lax.ppermute(maps, "sp", [(i, (i + s) % count) for i in range(count)])
        for s in range(1, count)
    ]
    return vmem_call(
        functools.partial(finish_kernel, head, count),
        jax.ShapeDtypeStruct((tokens, width), BF16),
        scalars=1,
        flops=4_000_000_000,
    )(
        place.astype(jnp.int32).reshape(1),
        jnp.stack(arrived),
        local, read_f, read_b,
        head_norm_gain.reshape(1, width),
    )


def body(
    layer_input,
    receptance,
    keys,
    values,
    erase_preact,
    decay_preact,
    decay_spike,
    head_norm_gain,
    output_weight,
    expert_norm_gain,
    routes,
    routing_weight,
    expert_gate_weight,
    expert_up_weight,
    expert_down_weight,
    shared_gate_weight,
    shared_up_weight,
    shared_down_weight,
):
    mixed = mixer(
        receptance, keys, values, erase_preact, decay_preact, decay_spike, head_norm_gain
    )
    row_count = layer_input.shape[0]
    model_width = layer_input.shape[1]
    slab = mixed
    projected = lax.psum_scatter(
        jnp.dot(slab, output_weight, preferred_element_type=jnp.float32).astype(jnp.bfloat16),
        "tp",
        scatter_dimension=0,
        tiled=True,
    ).astype(jnp.float32)
    residual = layer_input.astype(jnp.float32) + projected
    normed = residual * lax.rsqrt(jnp.mean(residual * residual, axis=-1, keepdims=True) + RMS_EPS)
    normed = (normed * expert_norm_gain.astype(jnp.float32)).astype(jnp.bfloat16)
    top_count = routes.shape[1]
    expert_local = expert_gate_weight.shape[0]
    sp_count = lax.axis_size("sp")
    expert_total = expert_local * sp_count
    capacity = max(2, (3 * row_count * top_count + 2 * expert_total - 1) // (2 * expert_total))
    slot_total = sp_count * capacity * expert_local
    entries = routes.reshape(-1)
    entry_count = entries.shape[0]
    expert_hot = (entries[:, None] == lax.broadcasted_iota(jnp.int32, (1, expert_total), 1)).astype(
        jnp.int32
    )
    rank_in = jnp.sum((jnp.cumsum(expert_hot, axis=0) - 1) * expert_hot, axis=1)
    slot_of = (entries // expert_local * capacity + rank_in) * expert_local + entries % expert_local
    slot_hot = (slot_of[:, None] == lax.broadcasted_iota(jnp.int32, (1, slot_total), 1)).astype(
        jnp.float32
    )
    owner_hot = (
        lax.broadcasted_iota(jnp.int32, (entry_count, 1), 0) // top_count
        == lax.broadcasted_iota(jnp.int32, (1, row_count), 1)
    ).astype(jnp.float32)
    placing = jnp.dot(slot_hot.T, owner_hot, precision=highest)
    weighting = jnp.dot(owner_hot.T, slot_hot * routing_weight.reshape(-1, 1), precision=highest)
    outgoing = jnp.dot(placing.astype(jnp.bfloat16), normed, preferred_element_type=jnp.float32)
    outgoing = outgoing.astype(jnp.bfloat16).reshape(sp_count, capacity, expert_local, model_width)
    arrived = lax.all_to_all(outgoing, "sp", split_axis=0, concat_axis=0, tiled=True)
    own_block = jnp.concatenate([arrived.reshape(slot_total, model_width), normed], axis=0)
    block_rows = own_block.shape[0]
    everyone = lax.all_gather(own_block, "tp", axis=0, tiled=True)
    slab = everyone
    slab = slab.reshape(block_rows * lax.axis_size("tp") // block_rows, block_rows, model_width)
    routed_in = slab[:, :slot_total].reshape(-1, expert_local, model_width)
    gate_value = jnp.einsum(
        "rjd,jdh->rjh", routed_in, expert_gate_weight, preferred_element_type=jnp.float32
    )
    up_value = jnp.einsum(
        "rjd,jdh->rjh", routed_in, expert_up_weight, preferred_element_type=jnp.float32
    )
    hidden = (jax.nn.silu(gate_value) * up_value).astype(jnp.bfloat16)
    routed_out = jnp.einsum(
        "rjh,jhd->rjd", hidden, expert_down_weight, preferred_element_type=jnp.float32
    )
    routed_out = routed_out.reshape(-1, slot_total, model_width)
    shared_in = slab[:, slot_total:].reshape(-1, model_width)
    shared_hidden = (
        jax.nn.silu(jnp.dot(shared_in, shared_gate_weight, preferred_element_type=jnp.float32))
        * jnp.dot(shared_in, shared_up_weight, preferred_element_type=jnp.float32)
    ).astype(jnp.bfloat16)
    shared_out = jnp.dot(shared_hidden, shared_down_weight, preferred_element_type=jnp.float32)
    shared_out = shared_out.reshape(-1, row_count, model_width)
    summed = lax.psum_scatter(
        jnp.concatenate([routed_out, shared_out], axis=1)
        .reshape(block_rows * lax.axis_size("tp"), model_width)
        .astype(jnp.bfloat16),
        "tp",
        scatter_dimension=0,
        tiled=True,
    ).astype(jnp.float32)
    routed_rows = (
        summed[:slot_total]
        .astype(jnp.bfloat16)
        .reshape(sp_count, capacity, expert_local, model_width)
    )
    returned = lax.all_to_all(routed_rows, "sp", split_axis=0, concat_axis=0, tiled=True)
    routed = jnp.dot(
        weighting, returned.reshape(slot_total, model_width).astype(jnp.float32), precision=highest
    )
    return (residual + summed[slot_total:] + routed).astype(jnp.bfloat16)


def solution(mesh):
    return jax.shard_map(
        body,
        mesh=mesh,
        in_specs=(
            P(("sp", "tp"), None),
            P("sp", "tp"),
            P("sp", "tp"),
            P("sp", "tp"),
            P("sp", "tp"),
            P("sp", "tp"),
            P("sp", "tp"),
            P("tp"),
            P("tp", None),
            P(),
            P(("sp", "tp"), None),
            P(("sp", "tp"), None),
            P("sp", None, "tp"),
            P("sp", None, "tp"),
            P("sp", "tp", None),
            P(None, "tp"),
            P(None, "tp"),
            P("tp", None),
        ),
        out_specs=P(("sp", "tp"), None),
        check_vma=False,
    )
```

```python
import functools
import jax
import jax.numpy as jnp
import numpy as np
from jax import lax
from jax.experimental import pallas as pl
from jax.experimental.pallas import tpu as pltpu
from jax.sharding import PartitionSpec as P

GN_EPS = 0.00064
RMS_EPS = 1e-06
LANES = 128
F32, BF16 = jnp.float32, jnp.bfloat16


def split(x):
    high = x.astype(BF16)
    return high, (x - high.astype(F32)).astype(BF16)


def dot(x, y):
    return jnp.dot(x, y, preferred_element_type=F32)


def dot_nt(x, y):
    return lax.dot_general(x, y, (((1,), (1,)), ((), ())), preferred_element_type=F32)


def head_of_lane(shape, head):
    return lax.broadcasted_iota(jnp.int32, shape, len(shape) - 1) // head


def expand(x, head):
    which = head_of_lane(x.shape, head)
    zero = jnp.zeros_like(x)
    return jnp.concatenate([jnp.where(which == h, x, zero) for h in range(x.shape[1] // head)], axis=0)


def wide(y, head):
    high, low = split(y)
    return jnp.concatenate([expand(high, head), expand(low, head)], axis=1)


def tall(x):
    high, low = split(x)
    return jnp.concatenate([high, low], axis=0)


def fold(out, rows, columns=LANES):
    return out[:rows, :columns] + (out[rows:, :columns] + out[:rows, columns:])


def times(x, y, head):
    return fold(dot(tall(x), wide(y, head)), x.shape[0])


def mixer_kernel(head, group, r_ref, k_ref, v_ref, e_ref, d_ref, s_ref,
                 loc_ref, rpf_ref, rpb_ref, maps_ref, ro_ref, pc_ref):
    tokens, width = k_ref.shape
    pairs, span = width // LANES, head
    per = LANES // head
    blocks = tokens // span
    row = lax.broadcasted_iota(jnp.int32, (span, LANES), 0)
    lane = lax.broadcasted_iota(jnp.int32, (span, LANES), 1)
    col = lane % head
    which = lane // head
    eye = (row == col).astype(F32)
    ones_bd = expand(jnp.ones((head, LANES), BF16), head)
    tri_row = lax.broadcasted_iota(jnp.int32, (span, span), 0)
    tri_col = lax.broadcasted_iota(jnp.int32, (span, span), 1)
    tri = (tri_row >= tri_col).astype(BF16)
    tri3 = jnp.concatenate([tri, tri, tri], axis=1)

    def prepare(at, p):
        lanes = slice(p * LANES, (p + 1) * LANES)
        rows = pl.ds(pl.multiple_of(at * span, span), span)
        keys = k_ref[rows, lanes].astype(F32)
        square = keys * keys
        total = dot(tall(square), ones_bd)
        unit = keys * lax.rsqrt(total[:span] + total[span:] + 1e-06)
        beta = unit / (1.0 + jnp.exp(-e_ref[rows, lanes].astype(F32)))
        spike = s_ref[rows, p * per:p * per + 1]
        for h in range(1, per):
            spike = jnp.where(which == h, s_ref[rows, p * per + h:p * per + h + 1], spike)
        log_decay = spike - 0.6065306597126334 / (1.0 + jnp.exp(-d_ref[rows, lanes].astype(F32)))
        high = log_decay.astype(BF16)
        rest = log_decay - high.astype(F32)
        mid = rest.astype(BF16)
        low = (rest - mid.astype(F32)).astype(BF16)
        cum = dot(tri3, jnp.concatenate([high, mid, low], axis=0))
        before = cum - log_decay
        centre, end = cum[span // 2 - 1:span // 2], cum[span - 1:span]
        e1, e0 = jnp.exp(cum - centre), jnp.exp(before - centre)
        i1, i0 = jnp.exp(centre - cum), jnp.exp(centre - before)
        fa, fb, fe = jnp.exp(centre), jnp.exp(end - centre), jnp.exp(end)
        read = r_ref[rows, lanes].astype(F32)
        forward = dict(u=unit * e0, r=read * e1, b=beta * i1, k=keys * i1, start=fa, total=fb)
        backward = dict(u=unit * i1, r=read * i0, b=beta * e0, k=keys * e0, start=fb, total=fa)
        for d, unit_of in ((0, forward), (1, backward)):
            unit_of.update(end=fe, v=v_ref[rows, lanes], at=at, p=p, d=d, lanes=lanes, rows=rows)
        return [forward, backward]

    same = [(row // (8 << i)) == (col // (8 << i)) for i in range(8) if (8 << i) <= span]
    strict = (row > col, row < col)
    incl = (row >= col, row <= col)

    def one_group(i, carry):
        units = []
        for g in range(group):
            for p in range(pairs):
                units += prepare(i * group + g, p)
        for q in units:
            left = tall(jnp.concatenate([q["u"], q["r"], eye * q["total"]], axis=0))
            bh, bl = split(q["b"])
            kh, kl = split(q["k"])
            right = jnp.concatenate([expand(x, head) for x in (bh, bl)], axis=0)
            out = fold(dot_nt(left, right), 3 * span)
            q["ub"] = jnp.where(strict[q["d"]], out[:span], 0.0)
            q["rb"] = jnp.where(incl[q["d"]], out[span:2 * span], 0.0)
            q["be"] = out[2 * span:]
            right = jnp.concatenate([expand(x, head) for x in (kh, kl)], axis=0)
            out = fold(dot_nt(left, right), 3 * span)
            q["uk"] = jnp.where(strict[q["d"]], out[:span], 0.0)
            q["rk"] = jnp.where(incl[q["d"]], out[span:2 * span], 0.0)
            q["ke"] = out[2 * span:]
        for q in units:
            q["D"] = jnp.where(same[0], q["ub"], 0.0)
            q["x"] = eye - q["D"]
        for q in units:
            q["D2"] = times(q["D"], q["D"], head)
        for q in units:
            left = jnp.concatenate([q["x"], q["D2"]], axis=0)
            out = times(left, q["D2"], head)
            q["x"], q["D4"] = q["x"] + out[:span], out[span:]
        for q in units:
            q["x"] = q["x"] + times(q["x"], q["D4"], head)
        for level in range(1, len(same)):
            for q in units:
                off = jnp.where(same[level] & ~same[level - 1], q["ub"], 0.0)
                q["t"] = times(q["x"], off, head)
            for q in units:
                q["x"] = q["x"] - times(q["t"], q["x"], head)
        for q in units:
            left = tall(jnp.concatenate([q["uk"], q["rk"], q["ke"]], axis=0))
            out = dot(left, expand(q["v"], head))
            out = out[:3 * span] + out[3 * span:]
            q["ukv"], q["rkv"], q["kev"] = out[:span], out[span:2 * span], out[2 * span:]
        for q in units:
            left = tall(q["x"])
            q["w"] = fold(dot(left, wide(q["u"] * q["start"], head)), span)
            q["y"] = fold(dot(left, wide(-q["ukv"], head)), span)
        for q in units:
            left = tall(jnp.concatenate([q["rb"], q["be"]], axis=0))
            ow = fold(dot(left, wide(q["w"], head)), 2 * span)
            oy = fold(dot(left, wide(q["y"], head)), 2 * span)
            readout = q["r"] * q["start"] - ow[:span]
            local = oy[:span] + q["rkv"]
            step = eye * q["end"] - ow[span:]
            carried = oy[span:] + q["kev"]
            at = (q["d"] * pairs + q["p"]) * blocks + q["at"]
            ro_ref[at, :span] = step
            ro_ref[at, span:] = readout
            pc_ref[at] = carried
            if q["d"] == 0:
                q_first = local
            else:
                loc_ref[q["rows"], q["lanes"]] = q_first + local
        return carry

    lax.fori_loop(0, blocks // group, one_group, 0)

    start = tuple(
        (jnp.zeros((span, LANES), F32), eye) for _ in range(2 * pairs)
    )

    def advance(i, states):
        after = []
        for c, (state, product) in enumerate(states):
            d, p = c // pairs, c % pairs
            at = i if d == 0 else blocks - 1 - i
            lanes = slice(p * LANES, (p + 1) * LANES)
            rows = pl.ds(pl.multiple_of(at * span, span), span)
            left = tall(ro_ref[c * blocks + at])
            zs = fold(dot(left, wide(state, head)), 2 * span)
            ps = fold(dot(left, wide(product, head)), 2 * span)
            loc_ref[rows, lanes] += zs[span:]
            (rpf_ref, rpb_ref)[d][rows, lanes] = ps[span:]
            after.append((zs[:span] + pc_ref[c * blocks + at], ps[:span]))
        return tuple(after)

    states = lax.fori_loop(0, blocks, advance, start)
    for c, (state, product) in enumerate(states):
        maps_ref[c, 0] = state.astype(BF16)
        maps_ref[c, 1] = product.astype(BF16)


def finish_kernel(head, count, span, place_ref, maps_ref, loc_ref, rpf_ref, rpb_ref, gain_ref,
                  own_ref, other_ref, mixed_ref):
    tokens, width = loc_ref.shape
    pairs = width // LANES
    place = place_ref[0]
    entries = []
    for c in range(2 * pairs):
        state = jnp.zeros((head, LANES), F32)
        for far in range(count - 1, 0, -1):
            s = far if c < pairs else count - far
            reached = (place >= far) if c < pairs else (place + far < count)
            out = dot(maps_ref[s - 1, c, 1], wide(state, head))
            new = out[:, :LANES] + out[:, LANES:] + maps_ref[s - 1, c, 0].astype(F32)
            state = jnp.where(reached, new, state)
        entries.append(state)
    mean_bd = expand(jnp.full((head, LANES), 1.0 / head, BF16), head)
    for p in range(pairs):
        lanes = slice(p * LANES, (p + 1) * LANES)
        mix = (
            loc_ref[:, lanes]
            + times(rpf_ref[:, lanes], entries[p], head)
            + times(rpb_ref[:, lanes], entries[pairs + p], head)
        )
        total = dot(tall(mix), mean_bd)
        away = mix - (total[:tokens] + total[tokens:])
        total = dot(tall(away * away), mean_bd)
        scaled = away * lax.rsqrt(total[:tokens] + total[tokens:] + GN_EPS)
        mixed_ref[:, lanes] = scaled * gain_ref[:, lanes].astype(F32)
    member = place_ref[1]
    for m in range(own_ref.shape[0] // span):
        for ref, flip in ((own_ref, 0), (other_ref, 1)):
            at = pl.multiple_of((member ^ (2 * m + flip)) * span, span)
            ref[m * span:(m + 1) * span] = mixed_ref[pl.ds(at, span)].astype(BF16)


def vmem_call(kernel, out_shape, scratch=(), scalars=0, flops=0, limit=20 << 20):
    many = isinstance(out_shape, (tuple, list))
    return lambda *args: pl.pallas_call(
        kernel,
        out_shape=out_shape,
        in_specs=[pl.BlockSpec(memory_space=pltpu.SMEM)] * scalars
        + [pl.BlockSpec(memory_space=pltpu.VMEM)] * (len(args) - scalars),
        out_specs=jax.tree.map(lambda _: pl.BlockSpec(memory_space=pltpu.VMEM), out_shape),
        scratch_shapes=list(scratch),
        compiler_params=pltpu.CompilerParams(vmem_limit_bytes=limit),
        cost_estimate=pl.CostEstimate(flops=flops, bytes_accessed=4 << 20, transcendentals=0),
    )(*args)


def mixer(receptance, keys, values, erase_preact, decay_preact, decay_spike, head_norm_gain, rows):
    tokens, width = keys.shape
    head = width // decay_spike.shape[1]
    pairs, blocks = width // LANES, tokens // head
    count, place = lax.axis_size("sp"), lax.axis_index("sp")
    shape = jax.ShapeDtypeStruct((tokens, width), F32)
    group = 2 if blocks % 2 == 0 else 1
    local, read_f, read_b, maps = vmem_call(
        functools.partial(mixer_kernel, head, group),
        (shape, shape, shape, jax.ShapeDtypeStruct((2 * pairs, 2, head, LANES), BF16)),
        [
            pltpu.VMEM((2 * pairs * blocks, 2 * head, LANES), F32),
            pltpu.VMEM((2 * pairs * blocks, head, LANES), F32),
        ],
        flops=20_000_000_000,
    )(receptance, keys, values, erase_preact, decay_preact, decay_spike)
    arrived = [
        lax.ppermute(maps, "sp", [(i, (i + s) % count) for i in range(count)])
        for s in range(1, count)
    ]
    return vmem_call(
        functools.partial(finish_kernel, head, count, rows),
        [jax.ShapeDtypeStruct((tokens // 2, width), BF16)] * 2,
        [pltpu.VMEM((tokens, width), F32)],
        scalars=1,
        flops=4_000_000_000,
    )(
        jnp.stack([place, lax.axis_index("tp")]).astype(jnp.int32),
        jnp.stack(arrived),
        local, read_f, read_b,
        head_norm_gain.reshape(1, width),
    )


def silu(v):
    return v / (1.0 + jnp.exp(-v))


def project_kernel(own_ref, mate_ref, wo_ref, wm_ref, *outs):
    rows, columns = outs[0].shape
    tile = min(512, columns)
    for n in range(columns // tile):
        cols = slice(n * tile, (n + 1) * tile)
        out = dot(own_ref[...], wo_ref[:, cols]) + dot(mate_ref[...], wm_ref[:, cols])
        for m, ref in enumerate(outs):
            ref[:, cols] = out[m * rows:(m + 1) * rows].astype(ref.dtype)


def norm_kernel(capacity, input_ref, gain_ref, routes_ref, weight_ref, *refs):
    parts, (residual_ref, ext_ref) = refs[:-2], refs[-2:]
    rows, columns = input_ref.shape
    residual = input_ref[...].astype(F32)
    for part in parts:
        residual += part[...].astype(F32)
    residual_ref[...] = residual
    scale = lax.rsqrt(jnp.mean(residual * residual, axis=1, keepdims=True) + RMS_EPS)
    ext_ref[:, :columns] = (residual * scale * gain_ref[...].astype(F32)).astype(BF16)
    lane = lax.broadcasted_iota(jnp.int32, (rows, LANES), 1)
    before = lax.broadcasted_iota(jnp.int32, (rows, rows), 0) > lax.broadcasted_iota(
        jnp.int32, (rows, rows), 1
    )
    top = routes_ref.shape[1]
    hot = [(routes_ref[:, k:k + 1] == lane).astype(F32) for k in range(top)]
    counts = dot(before.astype(BF16), sum(hot).astype(BF16))
    info = jnp.zeros((rows, LANES), F32)
    for k in range(top):
        rank = jnp.sum(counts * hot[k], axis=1, keepdims=True)
        code = routes_ref[:, k:k + 1].astype(F32) * capacity + rank
        info = jnp.where(lane == k, code, info)
        rest = weight_ref[:, k:k + 1]
        for piece in range(3):
            part = rest.astype(BF16).astype(F32)
            info = jnp.where(lane == top + 3 * k + piece, part, info)
            rest = rest - part
    ext_ref[:, columns:] = info.astype(BF16)


def slot_targets(group_ref, table_ref, groups, per_group):
    target = table_ref[0:1]
    for s in range(groups):
        base = (group_ref[0] ^ s) * per_group
        target = target + jnp.where(table_ref[2:3] == s, base, 0)
    return target.astype(F32), table_ref[1:2]


def slot_hits(info, target, block_of, k):
    rows = info.shape[0]
    block = lax.broadcasted_iota(jnp.int32, (rows, target.shape[1]), 0) // (rows // 2)
    return (info[:, k:k + 1] == target) & (block == block_of)


def dispatch_kernel(per_group, top, group_ref, table_ref, first_ref, second_ref, *outs):
    rows, columns = outs[0].shape
    info = jnp.concatenate([first_ref[:, columns:], second_ref[:, columns:]], axis=0).astype(F32)
    target, block_of = slot_targets(group_ref, table_ref, len(outs), per_group)
    hot = jnp.zeros((info.shape[0], target.shape[1]), F32)
    for k in range(top):
        hot = jnp.where(slot_hits(info, target, block_of, k), 1.0, hot)
    hot = hot.T.astype(BF16)
    tile = min(512, columns)
    for n in range(columns // tile):
        cols = slice(n * tile, (n + 1) * tile)
        both = jnp.concatenate([first_ref[:, cols], second_ref[:, cols]], axis=0)
        out = dot(hot, both).astype(BF16)
        for s, ref in enumerate(outs):
            ref[:, cols] = out[s * rows:(s + 1) * rows]


def combine_kernel(per_group, top, groups, group_ref, table_ref, first_ref, second_ref, shared_ref, *refs):
    arrived, outs = refs[:groups], refs[groups:]
    rows, columns = outs[0].shape
    info = jnp.concatenate([first_ref[:, columns:], second_ref[:, columns:]], axis=0).astype(F32)
    target, block_of = slot_targets(group_ref, table_ref, groups, per_group)
    weights = jnp.zeros((info.shape[0], target.shape[1]), F32)
    for k in range(top):
        at = top + 3 * k
        value = info[:, at:at + 1] + info[:, at + 1:at + 2] + info[:, at + 2:at + 3]
        weights = jnp.where(slot_hits(info, target, block_of, k), value, weights)
    high, low = split(weights)
    tile = min(512, columns)
    for n in range(columns // tile):
        cols = slice(n * tile, (n + 1) * tile)
        values = jnp.concatenate([ref[:, cols] for ref in arrived], axis=0)
        out = dot(high, values) + dot(low, values) + shared_ref[:, cols]
        for m, ref in enumerate(outs):
            ref[:, cols] = out[m * rows:(m + 1) * rows].astype(ref.dtype)


def final_kernel(residual_ref, own_ref, *refs):
    total = residual_ref[...] + own_ref[...]
    for ref in refs[:-1]:
        total += ref[...].astype(F32)
    refs[-1][...] = total.astype(BF16)


def experts_kernel(count, rows, columns, *refs):
    inputs, weights, outs, (x_ref, acc_ref) = (
        refs[:count], refs[count:count + 6], refs[count + 6:-2], refs[-2:]
    )
    expert, step = pl.program_id(0), pl.program_id(1)
    start = pl.multiple_of(expert * rows, rows)

    @pl.when(step == 0)
    def _():
        for i, ref in enumerate(inputs):
            x_ref[i * rows:(i + 1) * rows] = ref[pl.ds(start, rows), :columns]

    x = x_ref[...]
    hidden = []
    for half in range(2):
        gate, up = dot(x, weights[half][0]), dot(x, weights[2 + half][0])
        hidden.append((silu(gate) * up).astype(BF16))
    tile = min(512, columns)
    for n in range(columns // tile):
        cols = slice(n * tile, (n + 1) * tile)
        out = dot(hidden[0], weights[4][0, :, cols]) + dot(hidden[1], weights[5][0, :, cols])

        @pl.when(step == 0)
        def _():
            acc_ref[:, cols] = out

        @pl.when(step > 0)
        def _():
            acc_ref[:, cols] += out

    @pl.when(step == pl.num_programs(1) - 1)
    def _():
        for i, ref in enumerate(outs):
            ref[pl.ds(start, rows)] = acc_ref[i * rows:(i + 1) * rows].astype(ref.dtype)


def experts(inputs, weights, rows, columns, dtype, micros):
    local, _, width = weights[0].shape
    tile = min(256, width)
    whole = lambda a: pl.BlockSpec(a.shape, lambda e, t: (0, 0))
    tall_spec = pl.BlockSpec((1, columns, tile), lambda e, t: (e, 0, t))
    flat_spec = pl.BlockSpec((1, tile, columns), lambda e, t: (e, t, 0))
    shape = jax.ShapeDtypeStruct((local * rows, columns), dtype)
    count = len(inputs)
    return pl.pallas_call(
        functools.partial(experts_kernel, count, rows, columns),
        grid=(local, width // tile),
        in_specs=[whole(a) for a in inputs] + [tall_spec] * 4 + [flat_spec] * 2,
        out_specs=[whole(shape)] * count,
        out_shape=[shape] * count,
        scratch_shapes=[
            pltpu.VMEM((count * rows, columns), BF16),
            pltpu.VMEM((count * rows, columns), F32),
        ],
        compiler_params=pltpu.CompilerParams(
            vmem_limit_bytes=48 << 20, dimension_semantics=("arbitrary", "arbitrary")
        ),
        cost_estimate=pl.CostEstimate(
            flops=int(micros * 1e9), bytes_accessed=12 * local * columns * width, transcendentals=0
        ),
    )(*inputs, *weights)


def body(
    layer_input,
    receptance,
    keys,
    values,
    erase_preact,
    decay_preact,
    decay_spike,
    head_norm_gain,
    output_weight,
    expert_norm_gain,
    routes,
    routing_weight,
    expert_gate_weight,
    expert_up_weight,
    expert_down_weight,
    shared_gate_weight,
    shared_up_weight,
    shared_down_weight,
):
    groups, members = lax.axis_size("sp"), lax.axis_size("tp")
    chips = members // 2
    group = lax.axis_index("sp").astype(jnp.int32).reshape(1)
    rows, columns = layer_input.shape
    top = routes.shape[1]
    local = expert_gate_weight.shape[0]
    total = local * groups
    capacity = max(2, (3 * rows * top + 2 * total - 1) // (2 * total))
    capacity = -(-capacity // 8) * 8

    def over_tp(array, m):
        return lax.ppermute(array, "tp", [(j, j ^ m) for j in range(members)])

    def over_sp(array, s):
        return lax.ppermute(array, "sp", [(i, i ^ s) for i in range(groups)])

    shared_gate_weight, shared_up_weight, shared_down_weight = (
        w[None] for w in (shared_gate_weight, shared_up_weight, shared_down_weight)
    )
    output_mate = over_tp(output_weight, 1)
    pair = lambda *ws: [x for w in ws for x in (w, over_tp(w, 1))]
    routed_weights = pair(expert_gate_weight, expert_up_weight, expert_down_weight)
    shared_weights = pair(shared_gate_weight, shared_up_weight, shared_down_weight)

    own, other = mixer(
        receptance, keys, values, erase_preact, decay_preact, decay_spike, head_norm_gain, rows
    )
    mate = over_tp(other, 1)
    block = lambda dtype: jax.ShapeDtypeStruct((rows, columns), dtype)
    parts = vmem_call(
        project_kernel, [block(F32)] + [block(BF16)] * (chips - 1), flops=3_000_000_000
    )(own, mate, output_weight, output_mate)
    parts = [parts[0]] + [over_tp(parts[m], 2 * m) for m in range(1, chips)]
    residual, ext = vmem_call(
        functools.partial(norm_kernel, capacity),
        (block(F32), jax.ShapeDtypeStruct((rows, columns + LANES), BF16)),
        flops=1_500_000_000,
    )(layer_input, expert_norm_gain.reshape(1, columns), routes, routing_weight, *parts)

    blocks = [ext] + [over_tp(ext, 2 * m) for m in range(1, chips)]
    per_group = local * capacity
    slot_rows = local * 2 * capacity
    slots = np.arange(groups * slot_rows)
    within = slots % slot_rows
    table = np.zeros((8, slots.size), np.int32)
    table[0] = within // (2 * capacity) * capacity + within % capacity
    table[1] = within // capacity % 2
    table[2] = slots // slot_rows
    table = jnp.asarray(table)
    slot_shape = jax.ShapeDtypeStruct((slot_rows, columns), BF16)

    sent = [
        vmem_call(
            functools.partial(dispatch_kernel, per_group, top),
            [slot_shape] * groups,
            scalars=1,
            flops=1_500_000_000,
        )(group, table, blocks[h], blocks[h + 1])
        for h in range(0, chips, 2)
    ]
    arrived = [[a[0]] + [over_sp(a[s], s) for s in range(1, groups)] for a in sent]
    shared = experts(blocks, shared_weights, rows, columns, F32, 8)
    done = [experts(a, routed_weights, 2 * capacity, columns, BF16, 10) for a in arrived]
    back = [[a[0]] + [over_sp(a[s], s) for s in range(1, groups)] for a in done]
    partial = []
    for h in range(0, chips, 2):
        partial += vmem_call(
            functools.partial(combine_kernel, per_group, top, groups),
            [block(F32 if h == 0 else BF16), block(BF16)],
            scalars=1,
            flops=2_000_000_000,
        )(group, table, blocks[h], blocks[h + 1], jnp.concatenate(shared[h:h + 2]), *back[h // 2])
    partial = [partial[0]] + [over_tp(partial[m], 2 * m) for m in range(1, chips)]
    return vmem_call(final_kernel, block(BF16), flops=1_000_000_000)(residual, *partial)


def solution(mesh):
    return jax.shard_map(
        body,
        mesh=mesh,
        in_specs=(
            P(("sp", "tp"), None),
            P("sp", "tp"),
            P("sp", "tp"),
            P("sp", "tp"),
            P("sp", "tp"),
            P("sp", "tp"),
            P("sp", "tp"),
            P("tp"),
            P("tp", None),
            P(),
            P(("sp", "tp"), None),
            P(("sp", "tp"), None),
            P("sp", None, "tp"),
            P("sp", None, "tp"),
            P("sp", "tp", None),
            P(None, "tp"),
            P(None, "tp"),
            P("tp", None),
        ),
        out_specs=P(("sp", "tp"), None),
        check_vma=False,
    )
```

```python
import functools
import jax
import jax.numpy as jnp
import numpy as np
from jax import lax
from jax.experimental import pallas as pl
from jax.experimental.pallas import tpu as pltpu
from jax.sharding import PartitionSpec as P

GN_EPS = 0.00064
RMS_EPS = 1e-06
LANES = 128
EXPERT_LIMIT = 10 << 20
F32, BF16 = jnp.float32, jnp.bfloat16


def split(x):
    high = x.astype(BF16)
    return high, (x - high.astype(F32)).astype(BF16)


def dot(x, y):
    return jnp.dot(x, y, preferred_element_type=F32)


def dot_nt(x, y):
    return lax.dot_general(x, y, (((1,), (1,)), ((), ())), preferred_element_type=F32)


def head_of_lane(shape, head):
    return lax.broadcasted_iota(jnp.int32, shape, len(shape) - 1) // head


def expand(x, head):
    which = head_of_lane(x.shape, head)
    zero = jnp.zeros_like(x)
    return jnp.concatenate([jnp.where(which == h, x, zero) for h in range(x.shape[1] // head)], axis=0)


def wide(y, head):
    high, low = split(y)
    return jnp.concatenate([expand(high, head), expand(low, head)], axis=1)


def tall(x):
    high, low = split(x)
    return jnp.concatenate([high, low], axis=0)


def fold(out, rows, columns=LANES):
    return out[:rows, :columns] + (out[rows:, :columns] + out[:rows, columns:])


def times(x, y, head):
    return fold(dot(tall(x), wide(y, head)), x.shape[0])


def mixer_kernel(head, group, place_ref, r_ref, k_ref, v_ref, e_ref, d_ref, s_ref,
                 loc_ref, rpf_ref, rpb_ref, *rest):
    maps_refs, (ro_ref, pc_ref) = rest[:-2], rest[-2:]
    tokens, width = k_ref.shape
    pairs, span = width // LANES, head
    per = LANES // head
    blocks = tokens // span
    row = lax.broadcasted_iota(jnp.int32, (span, LANES), 0)
    lane = lax.broadcasted_iota(jnp.int32, (span, LANES), 1)
    col = lane % head
    which = lane // head
    eye = (row == col).astype(F32)
    ones_bd = expand(jnp.ones((head, LANES), BF16), head)
    tri_row = lax.broadcasted_iota(jnp.int32, (span, span), 0)
    tri_col = lax.broadcasted_iota(jnp.int32, (span, span), 1)
    tri = (tri_row >= tri_col).astype(BF16)
    tri3 = jnp.concatenate([tri, tri, tri], axis=1)

    def prepare(at, p):
        lanes = slice(p * LANES, (p + 1) * LANES)
        rows = pl.ds(pl.multiple_of(at * span, span), span)
        keys = k_ref[rows, lanes].astype(F32)
        square = keys * keys
        total = dot(tall(square), ones_bd)
        unit = keys * lax.rsqrt(total[:span] + total[span:] + 1e-06)
        beta = unit / (1.0 + jnp.exp(-e_ref[rows, lanes].astype(F32)))
        spike = s_ref[rows, p * per:p * per + 1]
        for h in range(1, per):
            spike = jnp.where(which == h, s_ref[rows, p * per + h:p * per + h + 1], spike)
        log_decay = spike - 0.6065306597126334 / (1.0 + jnp.exp(-d_ref[rows, lanes].astype(F32)))
        high = log_decay.astype(BF16)
        rest = log_decay - high.astype(F32)
        mid = rest.astype(BF16)
        low = (rest - mid.astype(F32)).astype(BF16)
        cum = dot(tri3, jnp.concatenate([high, mid, low], axis=0))
        before = cum - log_decay
        centre, end = cum[span // 2 - 1:span // 2], cum[span - 1:span]
        e1, e0 = jnp.exp(cum - centre), jnp.exp(before - centre)
        i1, i0 = jnp.exp(centre - cum), jnp.exp(centre - before)
        fa, fb, fe = jnp.exp(centre), jnp.exp(end - centre), jnp.exp(end)
        read = r_ref[rows, lanes].astype(F32)
        forward = dict(u=unit * e0, r=read * e1, b=beta * i1, k=keys * i1, start=fa, total=fb)
        backward = dict(u=unit * i1, r=read * i0, b=beta * e0, k=keys * e0, start=fb, total=fa)
        for d, unit_of in ((0, forward), (1, backward)):
            unit_of.update(end=fe, v=v_ref[rows, lanes], at=at, p=p, d=d, lanes=lanes, rows=rows)
        return [forward, backward]

    same = [(row // (8 << i)) == (col // (8 << i)) for i in range(8) if (8 << i) <= span]
    strict = (row > col, row < col)
    incl = (row >= col, row <= col)

    def one_group(i, carry):
        units = []
        for g in range(group):
            for p in range(pairs):
                units += prepare(i * group + g, p)
        for q in units:
            left = tall(jnp.concatenate([q["u"], q["r"], eye * q["total"]], axis=0))
            bh, bl = split(q["b"])
            kh, kl = split(q["k"])
            right = jnp.concatenate([expand(x, head) for x in (bh, bl)], axis=0)
            out = fold(dot_nt(left, right), 3 * span)
            q["ub"] = jnp.where(strict[q["d"]], out[:span], 0.0)
            q["rb"] = jnp.where(incl[q["d"]], out[span:2 * span], 0.0)
            q["be"] = out[2 * span:]
            right = jnp.concatenate([expand(x, head) for x in (kh, kl)], axis=0)
            out = fold(dot_nt(left, right), 3 * span)
            q["uk"] = jnp.where(strict[q["d"]], out[:span], 0.0)
            q["rk"] = jnp.where(incl[q["d"]], out[span:2 * span], 0.0)
            q["ke"] = out[2 * span:]
        for q in units:
            q["D"] = jnp.where(same[0], q["ub"], 0.0)
            q["x"] = eye - q["D"]
        for q in units:
            q["D2"] = times(q["D"], q["D"], head)
        for q in units:
            left = jnp.concatenate([q["x"], q["D2"]], axis=0)
            out = times(left, q["D2"], head)
            q["x"], q["D4"] = q["x"] + out[:span], out[span:]
        for q in units:
            q["x"] = q["x"] + times(q["x"], q["D4"], head)
        for level in range(1, len(same)):
            for q in units:
                off = jnp.where(same[level] & ~same[level - 1], q["ub"], 0.0)
                q["t"] = times(q["x"], off, head)
            for q in units:
                q["x"] = q["x"] - times(q["t"], q["x"], head)
        for q in units:
            left = tall(jnp.concatenate([q["uk"], q["rk"], q["ke"]], axis=0))
            out = dot(left, expand(q["v"], head))
            out = out[:3 * span] + out[3 * span:]
            q["ukv"], q["rkv"], q["kev"] = out[:span], out[span:2 * span], out[2 * span:]
        for q in units:
            left = tall(q["x"])
            q["w"] = fold(dot(left, wide(q["u"] * q["start"], head)), span)
            q["y"] = fold(dot(left, wide(-q["ukv"], head)), span)
        for q in units:
            left = tall(jnp.concatenate([q["rb"], q["be"]], axis=0))
            ow = fold(dot(left, wide(q["w"], head)), 2 * span)
            oy = fold(dot(left, wide(q["y"], head)), 2 * span)
            readout = q["r"] * q["start"] - ow[:span]
            local = oy[:span] + q["rkv"]
            step = eye * q["end"] - ow[span:]
            carried = oy[span:] + q["kev"]
            at = (q["d"] * pairs + q["p"]) * blocks + q["at"]
            ro_ref[at, :span] = step
            ro_ref[at, span:] = readout
            pc_ref[at] = carried
            if q["d"] == 0:
                q_first = local
            else:
                loc_ref[q["rows"], q["lanes"]] = q_first + local
        return carry

    lax.fori_loop(0, blocks // group, one_group, 0)

    start = tuple(
        (jnp.zeros((span, LANES), F32), eye) for _ in range(2 * pairs)
    )

    def advance(i, states):
        after = []
        for c, (state, product) in enumerate(states):
            d, p = c // pairs, c % pairs
            at = i if d == 0 else blocks - 1 - i
            lanes = slice(p * LANES, (p + 1) * LANES)
            rows = pl.ds(pl.multiple_of(at * span, span), span)
            left = tall(ro_ref[c * blocks + at])
            zs = fold(dot(left, wide(state, head)), 2 * span)
            ps = fold(dot(left, wide(product, head)), 2 * span)
            loc_ref[rows, lanes] += zs[span:]
            (rpf_ref, rpb_ref)[d][rows, lanes] = ps[span:]
            after.append((zs[:span] + pc_ref[c * blocks + at], ps[:span]))
        return tuple(after)

    states = lax.fori_loop(0, blocks, advance, start)
    place = place_ref[0]
    for s, ref in enumerate(maps_refs, 1):
        later = (place ^ s) > place
        for p in range(pairs):
            for n in range(2):
                ref[p, n] = jnp.where(later, states[p][n], states[pairs + p][n]).astype(BF16)


def finish_kernel(head, count, span, place_ref, loc_ref, rpf_ref, rpb_ref, gain_ref, *rest):
    maps_refs, (own_ref, other_ref, mixed_ref, maps_ref) = rest[:-4], rest[-4:]
    tokens, width = loc_ref.shape
    pairs = width // LANES
    place = place_ref[0]
    for s, ref in enumerate(maps_refs, 1):
        maps_ref[s] = ref[...]
    maps_ref[0] = jnp.zeros_like(maps_ref[0])
    states = [jnp.zeros((head, LANES), F32)] * (2 * pairs)
    for step in range(count - 1):
        for c in range(2 * pairs):
            at = step if c < pairs else count - 1 - step
            passed = (at < place) if c < pairs else (at > place)
            s = place ^ at
            out = dot(maps_ref[s, c % pairs, 1], wide(states[c], head))
            new = out[:, :LANES] + out[:, LANES:] + maps_ref[s, c % pairs, 0].astype(F32)
            states[c] = jnp.where(passed, new, states[c])
    entries = states
    mean_bd = expand(jnp.full((head, LANES), 1.0 / head, BF16), head)
    for p in range(pairs):
        lanes = slice(p * LANES, (p + 1) * LANES)
        mix = (
            loc_ref[:, lanes]
            + times(rpf_ref[:, lanes], entries[p], head)
            + times(rpb_ref[:, lanes], entries[pairs + p], head)
        )
        total = dot(tall(mix), mean_bd)
        away = mix - (total[:tokens] + total[tokens:])
        total = dot(tall(away * away), mean_bd)
        scaled = away * lax.rsqrt(total[:tokens] + total[tokens:] + GN_EPS)
        mixed_ref[:, lanes] = scaled * gain_ref[:, lanes].astype(F32)
    member = place_ref[1]
    for m in range(own_ref.shape[0] // span):
        for ref, flip in ((own_ref, 0), (other_ref, 1)):
            at = pl.multiple_of((member ^ (2 * m + flip)) * span, span)
            ref[m * span:(m + 1) * span] = mixed_ref[pl.ds(at, span)].astype(BF16)


def vmem_call(kernel, out_shape, scratch=(), scalars=0, flops=0, limit=8 << 20, keep=()):
    def without(given):
        return lambda *refs: kernel(*refs[:given], *refs[given + len(keep):])

    return lambda *args: pl.pallas_call(
        without(len(args)),
        out_shape=out_shape,
        in_specs=[pl.BlockSpec(memory_space=pltpu.SMEM)] * scalars
        + [pl.BlockSpec(memory_space=pltpu.VMEM)] * (len(args) - scalars)
        + [pl.BlockSpec(memory_space=pl.ANY)] * len(keep),
        out_specs=jax.tree.map(lambda _: pl.BlockSpec(memory_space=pltpu.VMEM), out_shape),
        scratch_shapes=list(scratch),
        compiler_params=pltpu.CompilerParams(vmem_limit_bytes=limit),
        cost_estimate=pl.CostEstimate(flops=flops, bytes_accessed=4 << 20, transcendentals=0),
    )(*args, *keep)


def mixer(receptance, keys, values, erase_preact, decay_preact, decay_spike, head_norm_gain, rows):
    tokens, width = keys.shape
    head = width // decay_spike.shape[1]
    pairs, blocks = width // LANES, tokens // head
    count, place = lax.axis_size("sp"), lax.axis_index("sp")
    shape = jax.ShapeDtypeStruct((tokens, width), F32)
    group = 4 if blocks % 4 == 0 else 1
    places = jnp.stack([place, lax.axis_index("tp")]).astype(jnp.int32)
    memory = lambda space: pl.BlockSpec(memory_space=space)
    maps = jax.ShapeDtypeStruct((pairs, 2, head, LANES), BF16)
    out_shape = (shape, shape, shape) + (maps,) * (count - 1)
    local, read_f, read_b, *maps = pl.pallas_call(
        functools.partial(mixer_kernel, head, group),
        out_shape=out_shape,
        in_specs=[memory(pltpu.SMEM)] + [memory(pltpu.VMEM)] * 6,
        out_specs=[memory(pltpu.VMEM)] * len(out_shape),
        scratch_shapes=[
            pltpu.VMEM((2 * pairs * blocks, 2 * head, LANES), F32),
            pltpu.VMEM((2 * pairs * blocks, head, LANES), F32),
        ],
        compiler_params=pltpu.CompilerParams(vmem_limit_bytes=20 << 20),
        cost_estimate=pl.CostEstimate(
            flops=20_000_000_000, bytes_accessed=4 << 20, transcendentals=0
        ),
    )(places, receptance, keys, values, erase_preact, decay_preact, decay_spike)
    arrived = [
        lax.ppermute(maps[s - 1], "sp", [(i, i ^ s) for i in range(count)])
        for s in range(1, count)
    ]
    return vmem_call(
        functools.partial(finish_kernel, head, count, rows),
        [jax.ShapeDtypeStruct((tokens // 2, width), BF16)] * 2,
        [
            pltpu.VMEM((tokens, width), F32),
            pltpu.VMEM((count, pairs, 2, head, LANES), BF16),
        ],
        scalars=1,
        flops=4_000_000_000,
    )(places, local, read_f, read_b, head_norm_gain.reshape(1, width), *arrived)


def silu(v):
    return v / (1.0 + jnp.exp(-v))


def project_kernel(own_ref, mate_ref, wo_ref, wm_ref, *outs):
    rows, columns = outs[0].shape
    tile = min(512, columns)
    for n in range(columns // tile):
        cols = slice(n * tile, (n + 1) * tile)
        out = dot(own_ref[...], wo_ref[:, cols]) + dot(mate_ref[...], wm_ref[:, cols])
        for m, ref in enumerate(outs):
            ref[:, cols] = out[m * rows:(m + 1) * rows].astype(ref.dtype)


def norm_kernel(capacity, input_ref, gain_ref, routes_ref, weight_ref, *refs):
    parts, (residual_ref, ext_ref) = refs[:-2], refs[-2:]
    rows, columns = input_ref.shape
    residual = input_ref[...].astype(F32)
    for part in parts:
        residual += part[...].astype(F32)
    residual_ref[...] = residual
    scale = lax.rsqrt(jnp.mean(residual * residual, axis=1, keepdims=True) + RMS_EPS)
    ext_ref[:, :columns] = (residual * scale * gain_ref[...].astype(F32)).astype(BF16)
    lane = lax.broadcasted_iota(jnp.int32, (rows, LANES), 1)
    before = lax.broadcasted_iota(jnp.int32, (rows, rows), 0) > lax.broadcasted_iota(
        jnp.int32, (rows, rows), 1
    )
    top = routes_ref.shape[1]
    hot = [(routes_ref[:, k:k + 1] == lane).astype(F32) for k in range(top)]
    counts = dot(before.astype(BF16), sum(hot).astype(BF16))
    info = jnp.zeros((rows, LANES), F32)
    for k in range(top):
        rank = jnp.sum(counts * hot[k], axis=1, keepdims=True)
        code = routes_ref[:, k:k + 1].astype(F32) * capacity + rank
        info = jnp.where(lane == k, code, info)
        rest = weight_ref[:, k:k + 1]
        for piece in range(3):
            part = rest.astype(BF16).astype(F32)
            info = jnp.where(lane == top + 3 * k + piece, part, info)
            rest = rest - part
    ext_ref[:, columns:] = info.astype(BF16)


def slot_targets(group_ref, table_ref, groups, per_group):
    target = table_ref[0:1]
    for s in range(groups):
        base = (group_ref[0] ^ s) * per_group
        target = target + jnp.where(table_ref[1:2] == s, base, 0)
    return target.astype(F32)


def dispatch_kernel(per_group, top, group_ref, table_ref, block_ref, *outs):
    rows, columns = outs[0].shape
    info = block_ref[:, columns:].astype(F32)
    target = slot_targets(group_ref, table_ref, len(outs), per_group)
    hot = jnp.zeros((info.shape[0], target.shape[1]), F32)
    for k in range(top):
        hot = jnp.where(info[:, k:k + 1] == target, 1.0, hot)
    hot = hot.T.astype(BF16)
    tile = min(512, columns)
    for n in range(columns // tile):
        cols = slice(n * tile, (n + 1) * tile)
        out = dot(hot, block_ref[:, cols])
        for s, ref in enumerate(outs):
            ref[:, cols] = out[s * rows:(s + 1) * rows].astype(BF16)


def combine_kernel(per_group, top, groups, group_ref, table_ref, block_ref, shared_ref, *refs):
    arrived, out_ref = refs[:groups], refs[groups]
    columns = out_ref.shape[1]
    info = block_ref[:, columns:].astype(F32)
    target = slot_targets(group_ref, table_ref, groups, per_group)
    weights = jnp.zeros((info.shape[0], target.shape[1]), F32)
    for k in range(top):
        at = top + 3 * k
        value = info[:, at:at + 1] + info[:, at + 1:at + 2] + info[:, at + 2:at + 3]
        weights = jnp.where(info[:, k:k + 1] == target, value, weights)
    high, low = split(weights)
    tile = min(512, columns)
    for n in range(columns // tile):
        cols = slice(n * tile, (n + 1) * tile)
        values = jnp.concatenate([ref[:, cols] for ref in arrived], axis=0)
        out = dot(high, values) + dot(low, values) + shared_ref[:, cols]
        out_ref[:, cols] = out.astype(out_ref.dtype)


def final_kernel(residual_ref, own_ref, *refs):
    total = residual_ref[...] + own_ref[...]
    for ref in refs[:-1]:
        total += ref[...].astype(F32)
    refs[-1][...] = total.astype(BF16)


def experts_kernel(count, rows, columns, after, *refs):
    inputs, refs = refs[:count], refs[count:]
    weights, refs = refs[:6], refs[6 + after:]
    outs, x_ref = refs[:-1], refs[-1]
    local, _, width = weights[0].shape
    part = min(256, width)
    tile = min(512, columns)
    for i, ref in enumerate(inputs):
        x_ref[i] = ref[:, :columns].astype(F32)

    def one_expert(expert, carry):
        at = pl.ds(pl.multiple_of(expert * rows, rows), rows)
        x = jnp.concatenate([x_ref[i, at] for i in range(count)], axis=0).astype(BF16)
        hidden = []
        for half in range(2):
            for t in range(width // part):
                cols = slice(t * part, (t + 1) * part)
                gate = dot(x, weights[half][expert, :, cols])
                up = dot(x, weights[2 + half][expert, :, cols])
                hidden.append((silu(gate) * up).astype(BF16))
        hidden = [
            jnp.concatenate(hidden[:width // part], axis=1),
            jnp.concatenate(hidden[width // part:], axis=1),
        ]
        for n in range(columns // tile):
            cols = slice(n * tile, (n + 1) * tile)
            out = dot(hidden[0], weights[4][expert, :, cols]) + dot(
                hidden[1], weights[5][expert, :, cols]
            )
            for i in range(count):
                x_ref[i, at, cols] = out[i * rows:(i + 1) * rows]
        return carry

    lax.fori_loop(0, local, one_expert, 0)
    for i, ref in enumerate(outs):
        ref[...] = x_ref[i].astype(ref.dtype)


def experts(inputs, weights, rows, columns, dtype, micros, after=()):
    local = weights[0].shape[0]
    shape = jax.ShapeDtypeStruct((local * rows, columns), dtype)
    count = len(inputs)
    return pl.pallas_call(
        functools.partial(experts_kernel, count, rows, columns, len(after)),
        in_specs=[pl.BlockSpec(memory_space=pltpu.VMEM)] * (count + 6)
        + [pl.BlockSpec(memory_space=pl.ANY)] * len(after),
        out_specs=[pl.BlockSpec(memory_space=pltpu.VMEM)] * count,
        out_shape=[shape] * count,
        scratch_shapes=[pltpu.VMEM((count, local * rows, columns), F32)],
        compiler_params=pltpu.CompilerParams(vmem_limit_bytes=EXPERT_LIMIT),
        cost_estimate=pl.CostEstimate(
            flops=int(micros * 1e9), bytes_accessed=1 << 20, transcendentals=0
        ),
    )(*inputs, *weights, *after)


def stage_kernel(*refs):
    count = (len(refs) - 1) // 2
    sems = refs[-1]
    copies = [
        pltpu.make_async_copy(refs[i], refs[count + i], sems.at[i]) for i in range(count)
    ]
    for copy in copies:
        copy.start()
    for copy in copies:
        copy.wait()


def stage(arrays, limit):
    return pl.pallas_call(
        stage_kernel,
        in_specs=[pl.BlockSpec(memory_space=pltpu.HBM)] * len(arrays),
        out_specs=[pl.BlockSpec(memory_space=pltpu.VMEM)] * len(arrays),
        out_shape=[jax.ShapeDtypeStruct(a.shape, a.dtype) for a in arrays],
        scratch_shapes=[pltpu.SemaphoreType.DMA((len(arrays),))],
        compiler_params=pltpu.CompilerParams(vmem_limit_bytes=limit),
        cost_estimate=pl.CostEstimate(flops=10_000_000_000, bytes_accessed=1 << 20, transcendentals=0),
    )(*arrays)


def turns(chips):
    last = list(range(1, chips)) + [0]
    return [last[i:i + 2] for i in range(0, chips, 2)]


def body(
    layer_input,
    receptance,
    keys,
    values,
    erase_preact,
    decay_preact,
    decay_spike,
    head_norm_gain,
    output_weight,
    expert_norm_gain,
    routes,
    routing_weight,
    expert_gate_weight,
    expert_up_weight,
    expert_down_weight,
    shared_gate_weight,
    shared_up_weight,
    shared_down_weight,
):
    groups, members = lax.axis_size("sp"), lax.axis_size("tp")
    chips = members // 2
    group = lax.axis_index("sp").astype(jnp.int32).reshape(1)
    rows, columns = layer_input.shape
    top = routes.shape[1]
    local = expert_gate_weight.shape[0]
    total = local * groups
    capacity = max(2, (3 * rows * top + 2 * total - 1) // (2 * total))
    capacity = -(-capacity // 8) * 8

    def over_tp(array, m):
        return lax.ppermute(array, "tp", [(j, j ^ m) for j in range(members)])

    def over_sp(array, s):
        return lax.ppermute(array, "sp", [(i, i ^ s) for i in range(groups)])

    shared_gate_weight, shared_up_weight, shared_down_weight = (
        w[None] for w in (shared_gate_weight, shared_up_weight, shared_down_weight)
    )
    output_mate = over_tp(output_weight, 1)
    pair = lambda *ws: [x for w in ws for x in (w, over_tp(w, 1))]
    routed_weights = pair(expert_gate_weight, expert_up_weight, expert_down_weight)
    shared_weights = pair(shared_gate_weight, shared_up_weight, shared_down_weight)

    own, other = mixer(
        receptance, keys, values, erase_preact, decay_preact, decay_spike, head_norm_gain, rows
    )
    mate = over_tp(other, 1)
    block = lambda dtype: jax.ShapeDtypeStruct((rows, columns), dtype)
    parts = vmem_call(
        project_kernel, [block(F32)] + [block(BF16)] * (chips - 1), flops=3_000_000_000
    )(own, mate, output_weight, output_mate)
    parts = list(parts)
    for m in range(1, chips):
        parts[m] = over_tp(parts[m], 2 * m)
    routed_weights = stage(routed_weights, 24 << 20)
    shared_weights = stage(shared_weights, 48 << 20)
    kept = tuple(routed_weights) + tuple(shared_weights)
    residual, ext = vmem_call(
        functools.partial(norm_kernel, capacity),
        (block(F32), jax.ShapeDtypeStruct((rows, columns + LANES), BF16)),
        flops=1_500_000_000,
        keep=kept,
    )(layer_input, expert_norm_gain.reshape(1, columns), routes, routing_weight, *parts)

    blocks = [ext]
    for m in range(1, chips):
        blocks.append(over_tp(ext, 2 * m))
    per_group = local * capacity
    slots = np.arange(groups * per_group)
    table = np.zeros((8, slots.size), np.int32)
    table[0] = slots % per_group
    table[1] = slots // per_group
    table = jnp.asarray(table)
    slot_shape = jax.ShapeDtypeStruct((per_group, columns), BF16)
    arrived = []
    for ext in blocks:
        sent = vmem_call(
            functools.partial(dispatch_kernel, per_group, top),
            [slot_shape] * groups,
            scalars=1,
            flops=700_000_000,
            keep=kept,
        )(group, table, ext)
        sent = list(sent)
        for s in range(1, groups):
            sent[s] = over_sp(sent[s], s)
        arrived.append(sent)
    back, after = {}, ()
    for served in turns(chips):
        rows_in = [a for i in served for a in arrived[i]]
        rows_out = experts(
            rows_in, routed_weights, capacity, columns, BF16, 7, after + tuple(shared_weights)
        )
        after = (rows_out[0],)
        for n, i in enumerate(served):
            mine = list(rows_out[n * groups:(n + 1) * groups])
            for s in range(1, groups):
                mine[s] = over_sp(mine[s], s)
            back[i] = mine
    shared = experts(blocks, shared_weights, rows, columns, F32, 3.5, after)
    partial = [
        vmem_call(
            functools.partial(combine_kernel, per_group, top, groups),
            block(F32 if i == 0 else BF16),
            scalars=1,
            flops=700_000_000,
        )(group, table, blocks[i], shared[i], *back[i])
        for i in range(chips)
    ]
    partial = [partial[0]] + [over_tp(partial[i], 2 * i) for i in range(1, chips)]
    return vmem_call(final_kernel, block(BF16), flops=1_000_000_000)(residual, *partial)


def solution(mesh):
    return jax.shard_map(
        body,
        mesh=mesh,
        in_specs=(
            P(("sp", "tp"), None),
            P("sp", "tp"),
            P("sp", "tp"),
            P("sp", "tp"),
            P("sp", "tp"),
            P("sp", "tp"),
            P("sp", "tp"),
            P("tp"),
            P("tp", None),
            P(),
            P(("sp", "tp"), None),
            P(("sp", "tp"), None),
            P("sp", None, "tp"),
            P("sp", None, "tp"),
            P("sp", "tp", None),
            P(None, "tp"),
            P(None, "tp"),
            P("tp", None),
        ),
        out_specs=P(("sp", "tp"), None),
        check_vma=False,
    )
```
